256 devices in a mesh: grp: 4 (over y, x), ep: 32 (over z), tp: 2 (over core).
Axes of the slice: x: 2, y: 2, z: 32, core: 2. Of those that a mesh axis runs over, the one named last changes fastest.
The devices are a block of a 4x8x32 slice.
Arguments:
- tokens: bfloat16 [8192, 2048], P(('grp', 'ep')), parts along dimension 0, may hold values from -6 to 6
- norm_gain: bfloat16 [2048], replicated, may hold values from 0.099609375 to 1.8984375
- routes: int32 [8192, 4], P(('grp', 'ep')), parts along dimension 0, may hold values from 0 to 31, all different within a row; in each aligned block of 64 rows (0 to 63, 64 to 127, ...) at most 16 rows name the same one
- route_weights: float32 [8192, 4], P(('grp', 'ep')), parts along dimension 0, may hold values from 0.2 to 1
- gate_experts: bfloat16 [32, 2048, 512], P('ep', None, 'tp'), may hold values from -0.125 to 0.125
- up_experts: bfloat16 [32, 2048, 512], P('ep', None, 'tp'), may hold values from -0.125 to 0.125
- down_experts: bfloat16 [32, 512, 2048], P('ep', 'tp'), may hold values from -0.25 to 0.25
- shared_gate: bfloat16 [2048, 512], P(None, 'tp'), may hold values from -0.125 to 0.125
- shared_up: bfloat16 [2048, 512], P(None, 'tp'), may hold values from -0.125 to 0.125
- shared_down: bfloat16 [512, 2048], P('tp'), may hold values from -0.25 to 0.25
- out_gain: bfloat16 [2048], P('tp'), may hold values from 0.099609375 to 1.8984375
Outputs:
- result: bfloat16 [8192, 2048], P(('grp', 'ep'), 'tp'), parts along dimension 0
The draws below stay inside these ranges and needn't reach their ends.
There are 4 independent parts, one for each index of `grp`. The reference program is written for one: setup_inputs(seed, part) draws one part's arguments, and reference() takes and returns one part's arrays. A program takes and returns all parts, laid end to end along the dimension named above; an argument that names none is the same for every part. Nothing has to cross between parts.
Inputs may be any that keep to these rules, and one draw needn't show every extreme that they name: `routes`: each row names 4 different experts. Among the 64 rows of one index of ep at most 16 name the same expert, and in every draw some expert is named by exactly 16 rows of some index.
All inputs are finite; a program needn't handle non-finite values.
Results may differ from the reference program's by a relative error of at most 0.0077.
Values may be sent and summed in bfloat16 or wider, within the bound.
No kernel may reach another device: no remote copies, remote signals or barrier semaphores. Data moves between devices by JAX's collectives and lax.ppermute only.
A program may use at most 64 MiB of HBM per device.

```python
import math
import jax
import jax.numpy as jnp
import numpy as np
from jax import lax

D = 2048
FF = 512
SF = 512
TOP_K = 4
TOK_DEV = 64
EXPERTS = 32
CAP = 16
TOKENS = 2048
N_TP = 2


def shard_levels(stream_key, extent, cuts, low, largest):
    def one(axis_at, blocks):
        heights = jax.random.uniform(jax.random.fold_in(jax.random.fold_in(stream_key, 6), axis_at), (blocks,), jnp.float32, low / len(cuts), largest / len(cuts))
        return jnp.repeat(jnp.exp(heights), extent[axis_at] // blocks).reshape((-1,) + (1,) * (len(extent) - axis_at - 1))

    level = one(*cuts[0])
    for cut in cuts[1:]:
        level = level * one(*cut)
    return level


def shared_out(own_key, own, number, rows, amount, top, limit, lean):
    sequence = jax.random.permutation(own_key, amount)
    packed, usual = shares(amount, rows * top, limit, lean, True), shares(amount, rows * top, limit, lean, False)
    places = jnp.arange(amount)

    def named(tallies, turn):
        used = int((tallies > 0).sum())
        fixed = max(1, used // 4)
        moved = fixed + (places - fixed + turn * (used - fixed)) % max(1, amount - fixed)
        return jnp.zeros((amount,), jnp.int32).at[sequence[jnp.where(places < fixed, places, moved)]].set(jnp.asarray(tallies, jnp.int32))

    tallies = jnp.where(number % 4 == 0, named(packed, number // 4), named(usual, number - number // 4 - 1))
    mixed = jax.random.permutation(jax.random.fold_in(own, 3), amount)
    giver, receiver = mixed[0:amount // 2 * 2:2], mixed[1:amount // 2 * 2:2]
    slack = jnp.minimum(tallies[giver] - 1, limit - tallies[receiver]) // 2
    slack = jnp.where((giver == sequence[0]) | (receiver == sequence[0]) | (tallies[receiver] == 0), 0, jnp.maximum(slack, 0))
    moved = jax.random.randint(jax.random.fold_in(own, 4), (amount // 2,), 0, 1 << 20) % (slack + 1)
    tallies = tallies.at[giver].add(-moved).at[receiver].add(moved)
    items = jnp.searchsorted(jnp.cumsum(tallies), jnp.arange(rows * top), side="right").astype(jnp.int32)
    listing = items.reshape(top, rows).T
    listing = listing[jax.random.permutation(jax.random.fold_in(own, 1), rows)]
    turn = jax.random.randint(jax.random.fold_in(own, 2), (rows, 1), 0, top)
    return jnp.take_along_axis(listing, (jnp.arange(top)[None, :] + turn) % top, axis=1)


def shares(count, total, bound, skew, full):
    loads = [(1 << 20) // math.isqrt(standing ** skew) + 1 for standing in range(1, count + 1)]
    largest = bound if full else min(bound, max(-(-total // count), total * loads[0] // sum(loads)))
    least = 1 if total - largest >= count - 1 else 0
    counts, spare = [largest] + [least] * (count - 1), total - largest - least * (count - 1)
    while spare > 0:
        candidates = [i for i in range(1, count) if counts[i] < largest] or [i for i in range(1, count) if counts[i] < bound]
        pool, left = sum([loads[i] for i in candidates]), spare
        for i in candidates:
            more = min(bound - counts[i], max(1, left * loads[i] // pool), spare)
            counts[i] = counts[i] + more
            spare = spare - more
    return np.array(counts)


def bell_draw(key, shape, deviation, most, shards=(), kind=jnp.bfloat16):
    result = jax.random.normal(key, shape, jnp.float32) * deviation
    if len(shards) > 0:
        result = shard_levels(key, shape, shards, -0.22, 0.18) * result
    return jnp.clip(result, min=-most, max=most).astype(kind)


def setup_inputs(seed: int = 0, part: int = 0) -> dict:
    keys = jax.random.split(jax.random.key(seed), 12)
    part_keys = jax.random.split(jax.random.fold_in(keys[11], part), 12)
    tokens = bell_draw(part_keys[0], (TOKENS, D), 1.0, 6.0, ((0, 32),))
    norm_gain = jnp.clip(1.0 + 0.18 * jax.random.normal(keys[1], (D,), jnp.float32), 0.099609375, 1.8984375).astype(jnp.bfloat16)
    routes_keys = jax.random.split(jax.random.fold_in(part_keys[2], 1), TOKENS // TOK_DEV)
    routes_turns = jax.random.permutation(jax.random.fold_in(part_keys[2], 3), TOKENS // TOK_DEV)
    routes = jax.vmap(lambda own, number: shared_out(jax.random.fold_in(part_keys[2], 2), own, number, TOK_DEV, EXPERTS, TOP_K, CAP, 2))(routes_keys, routes_turns).reshape((TOKENS, TOP_K))
    route_weights = jnp.clip(0.2 + 0.8 * jax.random.uniform(part_keys[3], (TOKENS, TOP_K), jnp.float32) ** shard_levels(part_keys[3], (TOKENS, TOP_K), ((0, 32),), -0.2, 0.2), 0.2, 1.0)
    gate_experts = bell_draw(keys[4], (EXPERTS, D, FF), D ** -0.5, 0.125, ((0, 32), (2, 2)))
    up_experts = bell_draw(keys[5], (EXPERTS, D, FF), D ** -0.5, 0.125, ((0, 32), (2, 2)))
    down_experts = bell_draw(keys[6], (EXPERTS, FF, D), FF ** -0.5, 0.25, ((0, 32), (1, 2)))
    shared_gate = bell_draw(keys[7], (D, SF), D ** -0.5, 0.125, ((1, 2),))
    shared_up = bell_draw(keys[8], (D, SF), D ** -0.5, 0.125, ((1, 2),))
    shared_down = bell_draw(keys[9], (SF, D), SF ** -0.5, 0.25, ((0, 2),))
    out_gain = jnp.clip(1.0 + 0.18 * jax.random.normal(keys[10], (D,), jnp.float32), 0.099609375, 1.8984375).astype(jnp.bfloat16)
    return dict(tokens=tokens, norm_gain=norm_gain, routes=routes, route_weights=route_weights, gate_experts=gate_experts, up_experts=up_experts, down_experts=down_experts, shared_gate=shared_gate, shared_up=shared_up, shared_down=shared_down, out_gain=out_gain)


EPS = 1e-06

def block_sum(activated, down_w):
    out_rows = activated.shape[0]
    block_width = activated.shape[1] // N_TP
    pieces = jnp.einsum('rtf,tfd->rtd', activated.reshape(out_rows, N_TP, block_width).astype(jnp.float32), down_w.reshape(N_TP, block_width, -1).astype(jnp.float32))
    rounded = lax.optimization_barrier(pieces.astype(jnp.bfloat16))
    return lax.optimization_barrier(jnp.sum(rounded.astype(jnp.float32), axis=1)).astype(jnp.bfloat16)

def swiglu_rows(normed, gate_w, up_w, down_w):
    gate_value = jnp.dot(normed, gate_w, preferred_element_type=jnp.float32)
    up_value = jnp.dot(normed, up_w, preferred_element_type=jnp.float32)
    activated = (jax.nn.silu(gate_value) * up_value).astype(jnp.bfloat16)
    return block_sum(activated, down_w)

def reference(tokens, norm_gain, routes, route_weights, gate_experts, up_experts, down_experts, shared_gate, shared_up, shared_down, out_gain):
    wide_tokens = tokens.astype(jnp.float32)
    normed = (wide_tokens * lax.rsqrt(lax.optimization_barrier(jnp.mean(wide_tokens * wide_tokens, axis=1, keepdims=True)) + EPS) * norm_gain.astype(jnp.float32)).astype(jnp.bfloat16)
    expert_total = gate_experts.shape[0]

    def expert_step(accum, inputs):
        gate_w, up_w, down_w, expert_id = inputs
        out_rows = swiglu_rows(normed, gate_w, up_w, down_w).astype(jnp.float32)
        weight_sum = lax.optimization_barrier(jnp.sum(jnp.where(routes == expert_id, route_weights, 0.0), axis=1))
        return (accum + weight_sum[:, None] * out_rows, None)
    start = jnp.zeros((tokens.shape[0], tokens.shape[1]), jnp.float32)
    routed, _ = lax.scan(expert_step, start, (gate_experts, up_experts, down_experts, jnp.arange(expert_total, dtype=jnp.int32)))
    shared = swiglu_rows(normed, shared_gate, shared_up, shared_down).astype(jnp.float32)
    mixed = shared + routed
    inverse = lax.rsqrt(lax.optimization_barrier(jnp.mean(mixed * mixed, axis=1, keepdims=True)) + EPS)
    return (mixed * inverse * out_gain.astype(jnp.float32)).astype(jnp.bfloat16)
```

```python
import functools

import jax
import jax.numpy as jnp
from jax import lax
from jax.experimental import pallas as pl
from jax.experimental.pallas import tpu as pltpu
from jax.sharding import PartitionSpec as P

EPS = 1e-06
CAP = 16
STRIDE = 4
META = 128
COLORS = 2
RCOLORS = 2
GROUPS = 2
INTERPRET = False


def moved(value, shift0, shift1):
    n = lax.axis_size("ep")
    pairs = []
    for i in range(n):
        for core, shift in enumerate((shift0, shift1)):
            if shift is not None:
                pairs.append((i * 2 + core, ((i + shift) % n) * 2 + core))
    return lax.ppermute(value, ("ep", "tp"), pairs)


def swapped(value):
    return lax.ppermute(value, "tp", [(0, 1), (1, 0)])


def pick(meta, ids, lanes):
    rows = meta.shape[0]
    lane = lax.broadcasted_iota(jnp.int32, (rows, lanes), 1)
    expert = jnp.full((rows, lanes), ids[-1], jnp.int32)
    for j in range(len(ids) - 2, -1, -1):
        expert = jnp.where(lane < CAP * (j + 1), ids[j], expert)
    expert = expert.astype(jnp.float32)
    named = meta[:, 0:1] == expert
    for k in range(1, 4):
        named = named | (meta[:, k : k + 1] == expert)
    named = jnp.where(named, 1.0, 0.0)
    earlier = lax.broadcasted_iota(jnp.int32, (rows, rows), 1) < lax.broadcasted_iota(
        jnp.int32, (rows, rows), 0
    )
    earlier = jnp.where(earlier, 1.0, 0.0).astype(jnp.bfloat16)
    rank = jnp.dot(earlier, named.astype(jnp.bfloat16), preferred_element_type=jnp.float32)
    slot = (lane % CAP).astype(jnp.float32)
    return jnp.where((rank == slot) & (named > 0), 1.0, 0.0).astype(jnp.bfloat16)


def take_rows(marks, chunk):
    return lax.dot_general(
        marks, chunk, (((0,), (0,)), ((), ())), preferred_element_type=jnp.float32
    ).astype(jnp.bfloat16)


def select_kernel(ids_ref, *refs):
    count = len(refs) - 6
    held = refs[: count + 1]
    self_ref, plus_ref, minus_ref, two_ref, marks_ref = refs[count + 1 :]
    width = held[0].shape[1]
    own_core0 = ids_ref[4] == 0
    ids = [ids_ref[j] for j in range(4)]
    for m in range(count):
        first, second = held[m][...], held[m + 1][...]
        main = jnp.where(own_core0, second, first)
        main_meta = main[:, width - META :].astype(jnp.float32)
        two_meta = first[:, width - META :].astype(jnp.float32)
        main_marks = pick(main_meta, ids[:3], 3 * CAP)
        two_marks = pick(two_meta, ids[3:], CAP)
        marks_ref[m, :, : 3 * CAP] = main_marks
        marks_ref[m, :, 3 * CAP :] = two_marks
        for start in range(0, width, 512):
            cols = slice(start, min(start + 512, width))
            rows = take_rows(main_marks, main[:, cols])
            out = slice(m * CAP, (m + 1) * CAP)
            self_ref[out, cols] = rows[:CAP]
            plus_ref[out, cols] = rows[CAP : 2 * CAP]
            minus_ref[out, cols] = rows[2 * CAP :]
            two_ref[out, cols] = take_rows(two_marks, first[:, cols])


def selected(ids, held):
    count = len(held) - 1
    rows, width = held[0].shape
    piece = jax.ShapeDtypeStruct((count * CAP, width), jnp.bfloat16)
    marks = jax.ShapeDtypeStruct((count, rows, 4 * CAP), jnp.bfloat16)
    vmem = pl.BlockSpec(memory_space=pltpu.VMEM)
    return pl.pallas_call(
        select_kernel,
        out_shape=(piece, piece, piece, piece, marks),
        in_specs=[pl.BlockSpec(memory_space=pltpu.SMEM)] + [vmem] * (count + 1),
        out_specs=[vmem] * 5,
        interpret=INTERPRET,
    )(ids, *held)


def combine_kernel(marks_ref, self_ref, plus_ref, minus_ref, two_ref, main_ref, second_ref):
    count = marks_ref.shape[0]
    width = self_ref.shape[1]
    for m in range(count):
        rows = slice(m * CAP, (m + 1) * CAP)
        marks = marks_ref[m]
        for start in range(0, width, 512):
            cols = slice(start, start + 512)
            back = jnp.concatenate(
                [self_ref[rows, cols], plus_ref[rows, cols], minus_ref[rows, cols]], axis=0
            )
            main_ref[m, :, cols] = jnp.dot(
                marks[:, : 3 * CAP], back, preferred_element_type=jnp.float32
            )
            second_ref[m, :, cols] = jnp.dot(
                marks[:, 3 * CAP :], two_ref[rows, cols], preferred_element_type=jnp.float32
            )


def combined(marks, pieces):
    count, rows, _ = marks.shape
    width = pieces[0].shape[1]
    sums = jax.ShapeDtypeStruct((count, rows, width), jnp.float32)
    vmem = pl.BlockSpec(memory_space=pltpu.VMEM)
    return pl.pallas_call(
        combine_kernel,
        out_shape=(sums, sums),
        in_specs=[vmem] * 5,
        out_specs=[vmem] * 2,
        interpret=INTERPRET,
    )(marks, *pieces)


def swiglu_part(rows, gate_w, up_w, down_w):
    gate_value = jnp.dot(rows, gate_w, preferred_element_type=jnp.float32)
    up_value = jnp.dot(rows, up_w, preferred_element_type=jnp.float32)
    activated = (jax.nn.silu(gate_value) * up_value).astype(jnp.bfloat16)
    return jnp.dot(activated, down_w, preferred_element_type=jnp.float32)


def short(value):
    return lax.reduce_precision(value, 8, 7)


def per_device(
    tokens,
    norm_gain,
    routes,
    route_weights,
    gate_experts,
    up_experts,
    down_experts,
    shared_gate,
    shared_up,
    shared_down,
    out_gain,
):
    tok_rows, model_width = tokens.shape
    n = lax.axis_size("ep")
    half_width = model_width // lax.axis_size("tp")
    hops = n // (2 * STRIDE)
    me = lax.axis_index("ep")
    core = lax.axis_index("tp")
    wide_tokens = tokens.astype(jnp.float32)
    normed = (
        wide_tokens
        * lax.rsqrt(jnp.mean(wide_tokens * wide_tokens, axis=1, keepdims=True) + EPS)
        * norm_gain.astype(jnp.float32)
    ).astype(jnp.bfloat16)

    high = short(route_weights)
    middle = short(route_weights - high)
    low = route_weights - high - middle
    meta = jnp.concatenate([routes.astype(jnp.float32), high, middle, low], axis=1)
    meta = jnp.pad(meta, ((0, 0), (0, META - meta.shape[1]))).astype(jnp.bfloat16)
    own = jnp.concatenate([normed, meta], axis=1)

    two = jnp.where(core == 0, 2, n - 2)
    ids = jnp.stack(
        [me, (me + 1) % n, (me + n - 1) % n, (me + two) % n, core, core, core, core]
    ).astype(jnp.int32)

    part = tok_rows // COLORS
    moving = [own[c * part : (c + 1) * part] for c in range(COLORS)]
    held = [own]
    for k in range(1, hops + 1):
        left = -STRIDE if k < hops else None
        moving = [moved(piece, STRIDE, left) for piece in moving]
        held.append(jnp.concatenate(moving, axis=0))

    per = hops // GROUPS
    gate_w, up_w, down_w = gate_experts[0], up_experts[0], down_experts[0]
    expert_id = me.astype(jnp.float32)
    marks, mains, seconds = [], [], []
    for g in range(GROUPS):
        to_self, to_plus, to_minus, to_two, mark = selected(ids, held[g * per : (g + 1) * per + 1])
        from_plus = moved(to_plus, 1, 1)
        from_minus = moved(to_minus, -1, -1)
        from_two = moved(to_two, 2, -2)
        mine = jnp.concatenate([to_self, from_plus, from_minus, from_two], axis=0)
        theirs = swapped(mine[:, :model_width])
        mine_meta = mine[:, model_width:].astype(jnp.float32)
        hit = (mine_meta[:, 0:4] == expert_id).astype(jnp.float32)
        weight = jnp.sum(
            hit * (mine_meta[:, 4:8] + mine_meta[:, 8:12] + mine_meta[:, 12:16]),
            axis=1,
            keepdims=True,
        )
        mine_part = swiglu_part(mine[:, :model_width], gate_w, up_w, down_w)
        their_part = swiglu_part(theirs, gate_w, up_w, down_w).astype(jnp.bfloat16)
        other_part = swapped(their_part).astype(jnp.float32)
        rows = ((mine_part + other_part) * weight).astype(jnp.bfloat16)
        rows = rows.reshape(4, per * CAP, model_width)
        pieces = (
            rows[0],
            moved(rows[1], -1, -1),
            moved(rows[2], 1, 1),
            moved(rows[3], -2, 2),
        )
        main, second = combined(mark, pieces)
        mains += [main[m] for m in range(per)]
        seconds += [second[m] for m in range(per)]

    zero = jnp.zeros((tok_rows, model_width), jnp.float32)
    padded = [zero] + mains + [zero]
    seconds = seconds + [zero]
    sums = [jnp.where(core == 0, padded[k], padded[k + 1]) + seconds[k] for k in range(hops + 1)]

    shared_partial = swiglu_part(normed, shared_gate, shared_up, shared_down)
    sums[0] = sums[0] + shared_partial
    width = model_width // RCOLORS
    finals = []
    for c in range(RCOLORS):
        cols = slice(c * width, (c + 1) * width)
        total = sums[hops][:, cols]
        for k in range(hops, 0, -1):
            right = STRIDE if k < hops else None
            total = sums[k - 1][:, cols] + moved(
                total.astype(jnp.bfloat16), -STRIDE, right
            ).astype(jnp.float32)
        finals.append(total)
    final = jnp.concatenate(finals, axis=1)

    sent = final.astype(jnp.bfloat16)
    mixed = final + swapped(sent).astype(jnp.float32)
    inverse = lax.rsqrt(jnp.mean(mixed * mixed, axis=1, keepdims=True) + EPS)
    kept = jnp.where(core == 0, mixed[:, :half_width], mixed[:, half_width:])
    return (kept * inverse * out_gain.astype(jnp.float32)[None, :]).astype(jnp.bfloat16)


def solution(mesh):
    in_specs = (
        P(("grp", "ep"), None),
        P(),
        P(("grp", "ep"), None),
        P(("grp", "ep"), None),
        P("ep", None, "tp"),
        P("ep", None, "tp"),
        P("ep", "tp", None),
        P(None, "tp"),
        P(None, "tp"),
        P("tp", None),
        P("tp"),
    )
    out_specs = P(("grp", "ep"), "tp")
    return jax.shard_map(
        per_device, mesh=mesh, in_specs=in_specs, out_specs=out_specs, check_vma=False
    )
```

```python
import functools

import jax
import jax.numpy as jnp
from jax import lax
from jax.experimental import pallas as pl
from jax.experimental.pallas import tpu as pltpu
from jax.sharding import PartitionSpec as P

EPS = 1e-06
CAP = 16
STRIDE = 5
HOPS = 2
META = 128
COLORS = 2
RCOLORS = 2
INTERPRET = False


def moved(value, shift0, shift1):
    n = lax.axis_size("ep")
    pairs = []
    for i in range(n):
        for core, shift in enumerate((shift0, shift1)):
            if shift is not None:
                pairs.append((i * 2 + core, ((i + shift) % n) * 2 + core))
    return lax.ppermute(value, ("ep", "tp"), pairs)


def swapped(value):
    return lax.ppermute(value, "tp", [(0, 1), (1, 0)])


def pick(meta, ids):
    rows, lanes = meta.shape[0], CAP * len(ids)
    lane = lax.broadcasted_iota(jnp.int32, (rows, lanes), 1)
    expert = jnp.full((rows, lanes), ids[-1], jnp.int32)
    for j in range(len(ids) - 2, -1, -1):
        expert = jnp.where(lane < CAP * (j + 1), ids[j], expert)
    expert = expert.astype(jnp.float32)
    named = jnp.zeros((rows, lanes), jnp.float32)
    high, low = named, named
    for k in range(4):
        hit = meta[:, k : k + 1] == expert
        named = jnp.where(hit, 1.0, named)
        high = jnp.where(hit, meta[:, 4 + k : 5 + k], high)
        low = jnp.where(hit, meta[:, 8 + k : 9 + k], low)
    earlier = lax.broadcasted_iota(jnp.int32, (rows, rows), 1) < lax.broadcasted_iota(
        jnp.int32, (rows, rows), 0
    )
    earlier = jnp.where(earlier, 1.0, 0.0).astype(jnp.bfloat16)
    rank = jnp.dot(earlier, named.astype(jnp.bfloat16), preferred_element_type=jnp.float32)
    marked = (rank == (lane % CAP).astype(jnp.float32)) & (named > 0)
    return tuple(
        jnp.where(marked, value, 0.0).astype(jnp.bfloat16) for value in (named, high, low)
    )


def take_rows(marks, chunk):
    return lax.dot_general(
        marks, chunk, (((0,), (0,)), ((), ())), preferred_element_type=jnp.float32
    ).astype(jnp.bfloat16)


PIECES = ("self", "near", "back", "near2", "back2", "far3", "far4", "far5", "extra")
SHIFTS = {"near": 1, "back": -1, "near2": 2, "back2": -2, "far3": 3, "far4": 4, "far5": 5}
TARGETS = (
    ("near", "near2"),
    ("self", "near", "back", "near2", "back2"),
    ("self", "near", "back", "near2", "back2", "far3", "far4", "far5"),
)


def slots():
    counts = {name: 0 for name in PIECES}
    table = []
    for names in TARGETS:
        table.append([(name, counts[name]) for name in names])
        for name in names:
            counts[name] += 1
    counts["extra"] = 1
    return table, counts


def select_kernel(ids_ref, *refs):
    held, outs, marks = refs[:3], dict(zip(PIECES, refs[3:12])), refs[12:]
    width = held[0].shape[1] - META
    core0 = ids_ref[len(PIECES)] == 0
    expert = {name: ids_ref[j] for j, name in enumerate(PIECES)}
    table, _ = slots()
    metas = [ref[:, width:].astype(jnp.float32) for ref in held]
    picked = [pick(metas[m], [expert[name] for name in TARGETS[m]]) for m in range(3)]
    picked.append(pick(jnp.where(core0, metas[2], metas[0]), [expert["extra"]]))
    for m in range(4):
        marks[m][0] = picked[m][1]
        marks[m][1] = picked[m][2]
    for start in range(0, width, 512):
        cols = slice(start, start + 512)
        for m in range(3):
            rows = take_rows(picked[m][0], held[m][:, cols])
            for j, (name, place) in enumerate(table[m]):
                outs[name][place * CAP : (place + 1) * CAP, cols] = rows[j * CAP : (j + 1) * CAP]
        mixed = jnp.where(core0, held[2][:, cols], held[0][:, cols])
        outs["extra"][:, cols] = take_rows(picked[3][0], mixed)


def selected(ids, held):
    rows, width = held[0].shape
    table, counts = slots()
    pieces = [
        jax.ShapeDtypeStruct((counts[name] * CAP, width - META), jnp.bfloat16) for name in PIECES
    ]
    marks = [
        jax.ShapeDtypeStruct((2, rows, CAP * count), jnp.bfloat16)
        for count in [len(names) for names in TARGETS] + [1]
    ]
    vmem = pl.BlockSpec(memory_space=pltpu.VMEM)
    out = pl.pallas_call(
        select_kernel,
        out_shape=pieces + marks,
        in_specs=[pl.BlockSpec(memory_space=pltpu.SMEM)] + [vmem] * 3,
        out_specs=[vmem] * 13,
        interpret=INTERPRET,
    )(ids, *held)
    return dict(zip(PIECES, out[:9])), out[9:]


def combine_kernel(core_ref, *refs):
    marks, pieces, sums = refs[:4], dict(zip(PIECES, refs[4:13])), refs[13:]
    width = pieces["self"].shape[1]
    table, _ = slots()
    core0 = core_ref[0] == 0
    for start in range(0, width, 512):
        cols = slice(start, start + 512)

        def weighed(m, rows):
            return jnp.dot(marks[m][0], rows, preferred_element_type=jnp.float32) + jnp.dot(
                marks[m][1], rows, preferred_element_type=jnp.float32
            )

        extra = weighed(3, pieces["extra"][:, cols])
        for m in range(3):
            rows = jnp.concatenate(
                [pieces[name][p * CAP : (p + 1) * CAP, cols] for name, p in table[m]], axis=0
            )
            total = weighed(m, rows)
            if m == 0:
                total = total + jnp.where(core0, 0.0, extra)
            if m == 2:
                total = total + jnp.where(core0, extra, 0.0)
            sums[m][:, cols] = total


def combined(core, marks, pieces):
    rows = marks[0].shape[1]
    sums = jax.ShapeDtypeStruct((rows, pieces["self"].shape[1]), jnp.float32)
    vmem = pl.BlockSpec(memory_space=pltpu.VMEM)
    return pl.pallas_call(
        combine_kernel,
        out_shape=(sums,) * 3,
        in_specs=[pl.BlockSpec(memory_space=pltpu.SMEM)] + [vmem] * 13,
        out_specs=[vmem] * 3,
        interpret=INTERPRET,
    )(core, *marks, *[pieces[name] for name in PIECES])


def swiglu_part(rows, gate_w, up_w, down_w):
    gate_value = jnp.dot(rows, gate_w, preferred_element_type=jnp.float32)
    up_value = jnp.dot(rows, up_w, preferred_element_type=jnp.float32)
    activated = (jax.nn.silu(gate_value) * up_value).astype(jnp.bfloat16)
    return jnp.dot(activated, down_w, preferred_element_type=jnp.float32)


def short(value):
    return lax.reduce_precision(value, 8, 7)


def per_device(
    tokens,
    norm_gain,
    routes,
    route_weights,
    gate_experts,
    up_experts,
    down_experts,
    shared_gate,
    shared_up,
    shared_down,
    out_gain,
):
    tok_rows, model_width = tokens.shape
    n = lax.axis_size("ep")
    half_width = model_width // lax.axis_size("tp")
    me = lax.axis_index("ep")
    core = lax.axis_index("tp")
    wide_tokens = tokens.astype(jnp.float32)
    normed = (
        wide_tokens
        * lax.rsqrt(jnp.mean(wide_tokens * wide_tokens, axis=1, keepdims=True) + EPS)
        * norm_gain.astype(jnp.float32)
    ).astype(jnp.bfloat16)

    high = short(route_weights)
    meta = jnp.concatenate([routes.astype(jnp.float32), high, route_weights - high], axis=1)
    meta = jnp.pad(meta, ((0, 0), (0, META - meta.shape[1]))).astype(jnp.bfloat16)
    own = jnp.concatenate([normed, meta], axis=1)

    sign = 1 - 2 * core
    last = n // 2 - HOPS * STRIDE
    shifts = [sign * SHIFTS.get(name, 0) for name in PIECES[:-1]]
    shifts.append(jnp.where(core == 0, last, 0))
    ids = jnp.stack([(me + n + shift) % n for shift in shifts] + [core]).astype(jnp.int32)

    def away(value, shift):
        return moved(value, shift, -shift)

    part = tok_rows // COLORS
    moving = [own[c * part : (c + 1) * part] for c in range(COLORS)]
    held = [own]
    for k in range(HOPS):
        moving = [away(piece, STRIDE) for piece in moving]
        held.append(jnp.concatenate(moving, axis=0))

    pieces, marks = selected(ids, held)
    extra = moved(pieces["extra"], last, None)
    arrived = {"self": pieces["self"], "extra": jnp.where(core == 0, extra, pieces["extra"])}
    for name in PIECES[-2:0:-1]:
        arrived[name] = away(pieces[name], SHIFTS[name])
    mine = jnp.concatenate([arrived[name] for name in PIECES], axis=0)
    theirs = swapped(mine)
    weights = gate_experts[0], up_experts[0], down_experts[0]
    their_part = swiglu_part(theirs, *weights).astype(jnp.bfloat16)
    other_part = swapped(their_part).astype(jnp.float32)
    rows = (swiglu_part(mine, *weights) + other_part).astype(jnp.bfloat16)
    _, counts = slots()
    done, at = {}, 0
    for name in PIECES:
        done[name] = rows[at : at + counts[name] * CAP]
        at += counts[name] * CAP
    extra = moved(done["extra"], -last, None)
    back = {"self": done["self"], "extra": jnp.where(core == 0, extra, done["extra"])}
    for name in PIECES[-2:0:-1]:
        back[name] = away(done[name], -SHIFTS[name])
    sums = list(combined(core.astype(jnp.int32)[None], marks, back))

    sums[0] = sums[0] + swiglu_part(normed, shared_gate, shared_up, shared_down)
    width = model_width // RCOLORS
    finals = []
    for c in range(RCOLORS):
        cols = slice(c * width, (c + 1) * width)
        total = sums[HOPS][:, cols]
        for k in range(HOPS - 1, -1, -1):
            came = away(total.astype(jnp.bfloat16), -STRIDE)
            total = sums[k][:, cols] + came.astype(jnp.float32)
        finals.append(total)
    final = jnp.concatenate(finals, axis=1)

    sent = final.astype(jnp.bfloat16)
    mixed = final + swapped(sent).astype(jnp.float32)
    inverse = lax.rsqrt(jnp.mean(mixed * mixed, axis=1, keepdims=True) + EPS)
    kept = jnp.where(core == 0, mixed[:, :half_width], mixed[:, half_width:])
    return (kept * inverse * out_gain.astype(jnp.float32)[None, :]).astype(jnp.bfloat16)


def solution(mesh):
    in_specs = (
        P(("grp", "ep"), None),
        P(),
        P(("grp", "ep"), None),
        P(("grp", "ep"), None),
        P("ep", None, "tp"),
        P("ep", None, "tp"),
        P("ep", "tp", None),
        P(None, "tp"),
        P(None, "tp"),
        P("tp", None),
        P("tp"),
    )
    out_specs = P(("grp", "ep"), "tp")
    return jax.shard_map(
        per_device, mesh=mesh, in_specs=in_specs, out_specs=out_specs, check_vma=False
    )
```

```python
import jax
import jax.numpy as jnp
from jax import lax
from jax.experimental import pallas as pl
from jax.experimental.pallas import tpu as pltpu
from jax.sharding import PartitionSpec as P

EPS = 1e-06
CAP = 16
STRIDE = 5
META = 128
BLOCK = 512
INTERPRET = False


def moved(value, shift0, shift1):
    n = lax.axis_size("ep")
    pairs = []
    for i in range(n):
        for core, shift in enumerate((shift0, shift1)):
            if shift is not None:
                pairs.append((i * 2 + core, ((i + shift) % n) * 2 + core))
    return lax.ppermute(value, ("ep", "tp"), pairs)


def swapped(value):
    return lax.ppermute(value, "tp", [(0, 1), (1, 0)])


def pick(meta, ids):
    rows, lanes = meta.shape[0], CAP * len(ids)
    lane = lax.broadcasted_iota(jnp.int32, (rows, lanes), 1)
    expert = jnp.full((rows, lanes), ids[-1], jnp.int32)
    for j in range(len(ids) - 2, -1, -1):
        expert = jnp.where(lane < CAP * (j + 1), ids[j], expert)
    expert = expert.astype(jnp.float32)
    named = jnp.zeros((rows, lanes), jnp.float32)
    high, low = named, named
    for k in range(4):
        hit = meta[:, k : k + 1] == expert
        named = jnp.where(hit, 1.0, named)
        high = jnp.where(hit, meta[:, 4 + k : 5 + k], high)
        low = jnp.where(hit, meta[:, 8 + k : 9 + k], low)
    earlier = lax.broadcasted_iota(jnp.int32, (rows, rows), 1) < lax.broadcasted_iota(
        jnp.int32, (rows, rows), 0
    )
    earlier = jnp.where(earlier, 1.0, 0.0).astype(jnp.bfloat16)
    rank = jnp.dot(earlier, named.astype(jnp.bfloat16), preferred_element_type=jnp.float32)
    marked = (rank == (lane % CAP).astype(jnp.float32)) & (named > 0)
    return tuple(
        jnp.where(marked, value, 0.0).astype(jnp.bfloat16) for value in (named, high, low)
    )


def take_rows(marks, chunk):
    return lax.dot_general(
        marks, chunk, (((0,), (0,)), ((), ())), preferred_element_type=jnp.float32
    ).astype(jnp.bfloat16)


SHIFTS = {"self": 0, "near": 1, "back": -1, "near2": 2, "back2": -2, "far3": 3, "far4": 4, "far5": 5}
NEAR = ("self", "near", "back", "near2", "back2")
FAR = NEAR + ("far3", "far4", "far5")
OWN = ("near", "near2")
SLOTS0 = {"self": 1, "near": 2, "back": 1, "near2": 2, "back2": 1}
SLOTS1 = {name: 1 for name in FAR + ("extra",)}
VMEM = pl.BlockSpec(memory_space=pltpu.VMEM)
SMEM = pl.BlockSpec(memory_space=pltpu.SMEM)


def bf16(*shape):
    return jax.ShapeDtypeStruct(shape, jnp.bfloat16)


def f32(*shape):
    return jax.ShapeDtypeStruct(shape, jnp.float32)


def call(kernel, outs, scalars, arrays):
    return pl.pallas_call(
        kernel,
        out_shape=tuple(outs),
        in_specs=[SMEM] * len(scalars) + [VMEM] * len(arrays),
        out_specs=tuple([VMEM] * len(outs)),
        interpret=INTERPRET,
    )(*scalars, *arrays)


def blocks(width):
    return [slice(start, start + BLOCK) for start in range(0, width, BLOCK)]


def norm_kernel(tokens_ref, gain_ref, routes_ref, weights_ref, low_ref, high_ref):
    rows, width = tokens_ref.shape
    half = rows // 2
    lane = lax.broadcasted_iota(jnp.int32, (half, META), 1)
    for ref, at in ((low_ref, 0), (high_ref, half)):
        part = slice(at, at + half)
        wide = tokens_ref[part, :].astype(jnp.float32)
        scale = lax.rsqrt(jnp.mean(wide * wide, axis=1, keepdims=True) + EPS)
        ref[:, :width] = (wide * scale * gain_ref[...].astype(jnp.float32)).astype(jnp.bfloat16)
        routes = routes_ref[part, :].astype(jnp.float32)
        weights = weights_ref[part, :]
        first = weights.astype(jnp.bfloat16).astype(jnp.float32)
        second = weights - first
        meta = jnp.zeros((half, META), jnp.float32)
        for k in range(routes.shape[1]):
            meta = jnp.where(lane == k, routes[:, k : k + 1], meta)
            meta = jnp.where(lane == 4 + k, first[:, k : k + 1], meta)
            meta = jnp.where(lane == 8 + k, second[:, k : k + 1], meta)
        ref[:, width:] = meta.astype(jnp.bfloat16)


def joined(pair, cols):
    return jnp.concatenate([pair[0][:, cols], pair[1][:, cols]], axis=0)


def meta_of(pair, width):
    return joined(pair, slice(width, width + META)).astype(jnp.float32)


def select0_kernel(ids_ref, own_a, own_b, one_a, one_b, *refs):
    outs, marks = dict(zip(NEAR, refs[:5])), refs[5:]
    own, one = (own_a, own_b), (one_a, one_b)
    width = own_a.shape[1] - META
    expert = {name: ids_ref[j] for j, name in enumerate(FAR)}
    from_own = pick(meta_of(own, width), [expert[name] for name in OWN])
    from_one = pick(meta_of(one, width), [expert[name] for name in NEAR])
    for ref, picked in zip(marks, (from_own, from_one)):
        ref[0] = picked[1]
        ref[1] = picked[2]
    for cols in blocks(width):
        rows = take_rows(from_own[0], joined(own, cols))
        for j, name in enumerate(OWN):
            outs[name][:CAP, cols] = rows[j * CAP : (j + 1) * CAP]
        rows = take_rows(from_one[0], joined(one, cols))
        for j, name in enumerate(NEAR):
            at = CAP if name in OWN else 0
            outs[name][at : at + CAP, cols] = rows[j * CAP : (j + 1) * CAP]


def select1_kernel(ids_ref, own_a, own_b, two_a, two_b, *refs):
    outs, extra, marks = dict(zip(FAR, refs[:8])), refs[8], refs[9:]
    own, two = (own_a, own_b), (two_a, two_b)
    width = own_a.shape[1] - META
    expert = {name: ids_ref[j] for j, name in enumerate(FAR)}
    core0 = ids_ref[len(FAR) + 1] == 0
    metas = meta_of(own, width), meta_of(two, width)
    from_two = pick(metas[1], [expert[name] for name in FAR])
    other = pick(jnp.where(core0, metas[0], metas[1]), [ids_ref[len(FAR)]])
    for ref, picked in zip(marks, (from_two, other)):
        ref[0] = picked[1]
        ref[1] = picked[2]
    for cols in blocks(width):
        chunk = joined(two, cols)
        rows = take_rows(from_two[0], chunk)
        for j, name in enumerate(FAR):
            outs[name][:, cols] = rows[j * CAP : (j + 1) * CAP]
        extra[:, cols] = take_rows(other[0], jnp.where(core0, joined(own, cols), chunk))


def weighed(marks, rows):
    return jnp.dot(marks[0], rows, preferred_element_type=jnp.float32) + jnp.dot(
        marks[1], rows, preferred_element_type=jnp.float32
    )


def combine1_kernel(ids_ref, marks, other, *refs):
    pieces, extra, sums = refs[:8], refs[8], refs[9:]
    core0 = ids_ref[len(FAR) + 1] == 0
    width = extra.shape[1]
    for cols in blocks(width):
        rows = jnp.concatenate([ref[:, cols] for ref in pieces], axis=0)
        total = weighed(marks, rows)
        total = total + jnp.where(core0, 0.0, weighed(other, extra[:, cols]))
        part = cols.start // (width // 2)
        at = cols.start - part * (width // 2)
        sums[part][:, at : at + BLOCK] = total.astype(jnp.bfloat16)


def combine0_kernel(ids_ref, mark_own, mark_one, other, *refs):
    pieces, extra, shared, own_sum, one_sum = dict(zip(NEAR, refs[:5])), *refs[5:]
    core0 = ids_ref[len(FAR) + 1] == 0
    for cols in blocks(extra.shape[1]):
        rows = jnp.concatenate([pieces[name][:CAP, cols] for name in OWN], axis=0)
        total = weighed(mark_own, rows) + shared[:, cols]
        own_sum[:, cols] = total + jnp.where(core0, weighed(other, extra[:, cols]), 0.0)
        rows = [
            pieces[name][CAP:, cols] if name in OWN else pieces[name][:, cols] for name in NEAR
        ]
        one_sum[:, cols] = weighed(mark_one, jnp.concatenate(rows, axis=0))


def ffn_kernel(rows_ref, gate_ref, up_ref, down_ref, out_ref):
    rows = rows_ref[...]
    gate_value = jnp.dot(rows, gate_ref[...], preferred_element_type=jnp.float32)
    up_value = jnp.dot(rows, up_ref[...], preferred_element_type=jnp.float32)
    activated = gate_value / (1.0 + jnp.exp(-gate_value)) * up_value
    activated = activated.astype(jnp.bfloat16)
    for cols in blocks(out_ref.shape[1]):
        out_ref[:, cols] = jnp.dot(
            activated, down_ref[:, cols], preferred_element_type=jnp.float32
        ).astype(out_ref.dtype)


def add_kernel(part_ref, other_ref, *outs):
    at = 0
    for ref in outs:
        rows = slice(at, at + ref.shape[0])
        ref[...] = (part_ref[rows, :] + other_ref[rows, :].astype(jnp.float32)).astype(jnp.bfloat16)
        at += ref.shape[0]


def expert_rows(slots, arrived, weights):
    mine = jnp.concatenate([arrived[name] for name in slots], axis=0)
    rows, width = mine.shape
    theirs = swapped(mine)
    (their_part,) = call(ffn_kernel, [bf16(rows, width)], [], [theirs, *weights])
    other_part = swapped(their_part)
    (my_part,) = call(ffn_kernel, [f32(rows, width)], [], [mine, *weights])
    outs = [bf16(count * CAP, width) for count in slots.values()]
    return dict(zip(slots, call(add_kernel, outs, [], [my_part, other_part])))


def away(value, shift):
    return moved(value, shift, -shift) if shift else value


def per_device(
    tokens,
    norm_gain,
    routes,
    route_weights,
    gate_experts,
    up_experts,
    down_experts,
    shared_gate,
    shared_up,
    shared_down,
    out_gain,
):
    tok_rows, width = tokens.shape
    n = lax.axis_size("ep")
    half_width = width // 2
    me = lax.axis_index("ep")
    core = lax.axis_index("tp")
    half = [bf16(tok_rows // 2, width + META)] * 2
    own = call(norm_kernel, half, [], [tokens, norm_gain[None, :], routes, route_weights])

    last = n // 2 - 2 * STRIDE
    sign = 1 - 2 * core
    shifts = [sign * SHIFTS[name] for name in FAR] + [jnp.where(core == 0, 0, -last)]
    ids = jnp.stack([(me + n + shift) % n for shift in shifts] + [core]).astype(jnp.int32)
    weights = gate_experts[0], up_experts[0], down_experts[0]

    one = [away(piece, STRIDE) for piece in own]
    two = [away(piece, STRIDE) for piece in one]
    marks = [(2, tok_rows, CAP * len(names)) for names in (OWN, NEAR, FAR, ("extra",))]
    marks = [bf16(*shape) for shape in marks]
    outs = [bf16(SLOTS0[name] * CAP, width) for name in NEAR]
    *pieces, mark_own, mark_one = call(select0_kernel, outs + marks[:2], [ids], [*own, *one])
    arrived0 = {name: away(piece, SHIFTS[name]) for name, piece in zip(NEAR, pieces)}
    outs = [bf16(CAP, width)] * 9
    *pieces, extra, mark_two, other = call(select1_kernel, outs + marks[2:], [ids], [*own, *two])
    arrived1 = {"extra": jnp.where(core == 0, extra, moved(extra, None, -last))}
    for name, piece in reversed(list(zip(FAR, pieces))):
        arrived1[name] = away(piece, SHIFTS[name])

    done0 = expert_rows(SLOTS0, arrived0, weights)
    done1 = expert_rows(SLOTS1, arrived1, weights)

    extra = jnp.where(core == 0, done1["extra"], moved(done1["extra"], None, last))
    back1 = {name: away(done1[name], -SHIFTS[name]) for name in reversed(FAR)}
    sums = call(
        combine1_kernel,
        [bf16(tok_rows, half_width)] * 2,
        [ids],
        [mark_two, other, *[back1[name] for name in FAR], extra],
    )
    came = [away(part, -STRIDE) for part in sums]
    back0 = [away(done0[name], -SHIFTS[name]) for name in NEAR]
    normed = jnp.concatenate([piece[:, :width] for piece in own], axis=0)
    (shared,) = call(
        ffn_kernel, [f32(tok_rows, width)], [], [normed, shared_gate, shared_up, shared_down]
    )
    own_sum, one_sum = call(
        combine0_kernel,
        [f32(tok_rows, width)] * 2,
        [ids],
        [mark_own, mark_one, other, *back0, extra, shared],
    )
    finals = []
    for c in range(2):
        cols = slice(c * half_width, (c + 1) * half_width)
        total = one_sum[:, cols] + came[c].astype(jnp.float32)
        total = away(total.astype(jnp.bfloat16), -STRIDE)
        finals.append(own_sum[:, cols] + total.astype(jnp.float32))
    final = jnp.concatenate(finals, axis=1)

    mixed = final + swapped(final.astype(jnp.bfloat16)).astype(jnp.float32)
    inverse = lax.rsqrt(jnp.mean(mixed * mixed, axis=1, keepdims=True) + EPS)
    kept = jnp.where(core == 0, mixed[:, :half_width], mixed[:, half_width:])
    return (kept * inverse * out_gain.astype(jnp.float32)[None, :]).astype(jnp.bfloat16)


def solution(mesh):
    in_specs = (
        P(("grp", "ep"), None),
        P(),
        P(("grp", "ep"), None),
        P(("grp", "ep"), None),
        P("ep", None, "tp"),
        P("ep", None, "tp"),
        P("ep", "tp", None),
        P(None, "tp"),
        P(None, "tp"),
        P("tp", None),
        P("tp"),
    )
    out_specs = P(("grp", "ep"), "tp")
    return jax.shard_map(
        per_device, mesh=mesh, in_specs=in_specs, out_specs=out_specs, check_vma=False
    )
```

```python
import jax
import jax.numpy as jnp
from jax import lax
from jax.experimental import pallas as pl
from jax.experimental.pallas import tpu as pltpu
from jax.sharding import PartitionSpec as P

EPS = 1e-06
CAP = 16
STRIDE = 6
META = 128
BLOCK = 512
SCOPED = 16 * 1024 * 1024
INTERPRET = False


def moved(value, shift0, shift1):
    n = lax.axis_size("ep")
    pairs = []
    for i in range(n):
        for core, shift in enumerate((shift0, shift1)):
            if shift is not None:
                pairs.append((i * 2 + core, ((i + shift) % n) * 2 + core))
    return lax.ppermute(value, ("ep", "tp"), pairs)


def swapped(value):
    return lax.ppermute(value, "tp", [(0, 1), (1, 0)])


def pick(meta, ids):
    rows, lanes = meta.shape[0], CAP * len(ids)
    lane = lax.broadcasted_iota(jnp.int32, (rows, lanes), 1)
    expert = jnp.full((rows, lanes), ids[-1], jnp.int32)
    for j in range(len(ids) - 2, -1, -1):
        expert = jnp.where(lane < CAP * (j + 1), ids[j], expert)
    expert = expert.astype(jnp.float32)
    named = jnp.zeros((rows, lanes), jnp.float32)
    high, low = named, named
    for k in range(4):
        hit = meta[:, k : k + 1] == expert
        named = jnp.where(hit, 1.0, named)
        high = jnp.where(hit, meta[:, 4 + k : 5 + k], high)
        low = jnp.where(hit, meta[:, 8 + k : 9 + k], low)
    earlier = lax.broadcasted_iota(jnp.int32, (rows, rows), 1) < lax.broadcasted_iota(
        jnp.int32, (rows, rows), 0
    )
    earlier = jnp.where(earlier, 1.0, 0.0).astype(jnp.bfloat16)
    rank = jnp.dot(earlier, named.astype(jnp.bfloat16), preferred_element_type=jnp.float32)
    marked = (rank == (lane % CAP).astype(jnp.float32)) & (named > 0)
    return tuple(
        jnp.where(marked, value, 0.0).astype(jnp.bfloat16) for value in (named, high, low)
    )


def take_rows(marks, chunk):
    return lax.dot_general(
        marks, chunk, (((0,), (0,)), ((), ())), preferred_element_type=jnp.float32
    ).astype(jnp.bfloat16)


SHIFTS = {"self": 0, "near": 1, "back": -1, "near2": 2, "back2": -2, "near3": 3}
NAMES = tuple(SHIFTS)
OWN = ("near", "near2", "near3")
SLOTS = {name: 3 if name in OWN else 2 for name in NAMES} | {"extra": 1}
VMEM = pl.BlockSpec(memory_space=pltpu.VMEM)
SMEM = pl.BlockSpec(memory_space=pltpu.SMEM)


def bf16(*shape):
    return jax.ShapeDtypeStruct(shape, jnp.bfloat16)


def f32(*shape):
    return jax.ShapeDtypeStruct(shape, jnp.float32)


def call(kernel, outs, scalars, arrays):
    return pl.pallas_call(
        kernel,
        out_shape=tuple(outs),
        in_specs=[SMEM] * len(scalars) + [VMEM] * len(arrays),
        out_specs=tuple([VMEM] * len(outs)),
        compiler_params=pltpu.CompilerParams(vmem_limit_bytes=SCOPED),
        interpret=INTERPRET,
    )(*scalars, *arrays)


def blocks(width):
    return [slice(start, start + BLOCK) for start in range(0, width, BLOCK)]


def norm_kernel(tokens_ref, gain_ref, routes_ref, weights_ref, low_ref, high_ref):
    rows, width = tokens_ref.shape
    half = rows // 2
    per_token = routes_ref.shape[0]
    weights = weights_ref[...]
    first = weights.astype(jnp.bfloat16)
    terms = (
        routes_ref[...].astype(jnp.float32).astype(jnp.bfloat16),
        first,
        (weights - first.astype(jnp.float32)).astype(jnp.bfloat16),
    )
    row = lax.broadcasted_iota(jnp.int32, (per_token, META), 0)
    lane = lax.broadcasted_iota(jnp.int32, (per_token, META), 1)
    meta = jnp.zeros((rows, META), jnp.float32)
    for j, term in enumerate(terms):
        place = jnp.where(lane == row + 4 * j, 1.0, 0.0).astype(jnp.bfloat16)
        meta = meta + lax.dot_general(
            term, place, (((0,), (0,)), ((), ())), preferred_element_type=jnp.float32
        )
    meta = meta.astype(jnp.bfloat16)
    for ref, at in ((low_ref, 0), (high_ref, half)):
        part = slice(at, at + half)
        wide = tokens_ref[part, :].astype(jnp.float32)
        scale = lax.rsqrt(jnp.mean(wide * wide, axis=1, keepdims=True) + EPS)
        ref[:, :width] = (wide * scale * gain_ref[...]).astype(jnp.bfloat16)
        ref[:, width:] = meta[part]


def joined(pair, cols):
    return jnp.concatenate([pair[0][:, cols], pair[1][:, cols]], axis=0)


def meta_of(pair, width):
    return joined(pair, slice(width, width + META)).astype(jnp.float32)


def select0_kernel(ids_ref, own_a, own_b, one_a, one_b, *refs):
    outs, marks = dict(zip(NAMES, refs[:6])), refs[6:]
    own, one = (own_a, own_b), (one_a, one_b)
    width = own_a.shape[1] - META
    expert = {name: ids_ref[j] for j, name in enumerate(NAMES)}
    from_own = pick(meta_of(own, width), [expert[name] for name in OWN])
    from_one = pick(meta_of(one, width), [expert[name] for name in NAMES])
    for ref, picked in zip(marks, (from_own, from_one)):
        ref[0] = picked[1]
        ref[1] = picked[2]
    for cols in blocks(width):
        rows = take_rows(from_own[0], joined(own, cols))
        for j, name in enumerate(OWN):
            outs[name][:CAP, cols] = rows[j * CAP : (j + 1) * CAP]
        rows = take_rows(from_one[0], joined(one, cols))
        for j, name in enumerate(NAMES):
            outs[name][-CAP:, cols] = rows[j * CAP : (j + 1) * CAP]


def select1_kernel(ids_ref, own_a, own_b, two_a, two_b, *refs):
    early, outs = dict(zip(NAMES, refs[:6])), dict(zip(NAMES, refs[6:12]))
    extra, marks = refs[12], refs[13:]
    own, two = (own_a, own_b), (two_a, two_b)
    width = own_a.shape[1] - META
    expert = {name: ids_ref[j] for j, name in enumerate(NAMES)}
    core0 = ids_ref[len(NAMES) + 1] == 0
    metas = meta_of(own, width), meta_of(two, width)
    from_two = pick(metas[1], [expert[name] for name in NAMES])
    other = pick(jnp.where(core0, metas[0], metas[1]), [ids_ref[len(NAMES)]])
    for ref, picked in zip(marks, (from_two, other)):
        ref[0] = picked[1]
        ref[1] = picked[2]
    for cols in blocks(width):
        chunk = joined(two, cols)
        rows = take_rows(from_two[0], chunk)
        for j, name in enumerate(NAMES):
            outs[name][:-CAP, cols] = early[name][:, cols]
            outs[name][-CAP:, cols] = rows[j * CAP : (j + 1) * CAP]
        extra[:, cols] = take_rows(other[0], jnp.where(core0, joined(own, cols), chunk))


def weighed(marks, rows):
    return jnp.dot(marks[0], rows, preferred_element_type=jnp.float32) + jnp.dot(
        marks[1], rows, preferred_element_type=jnp.float32
    )


def combine1_kernel(ids_ref, marks, other, *refs):
    pieces, extra, sums = refs[:6], refs[6], refs[7:]
    core0 = ids_ref[len(NAMES) + 1] == 0
    width = extra.shape[1]
    for cols in blocks(width):
        rows = jnp.concatenate([ref[-CAP:, cols] for ref in pieces], axis=0)
        total = weighed(marks, rows)
        total = total + jnp.where(core0, 0.0, weighed(other, extra[:, cols]))
        part = cols.start // (width // 2)
        at = cols.start - part * (width // 2)
        sums[part][:, at : at + BLOCK] = total.astype(jnp.bfloat16)


def combine0_kernel(ids_ref, mark_own, mark_one, other, *refs):
    pieces, extra, shared, own_sum, one_sum = dict(zip(NAMES, refs[:6])), *refs[6:]
    core0 = ids_ref[len(NAMES) + 1] == 0
    for cols in blocks(extra.shape[1]):
        rows = jnp.concatenate([pieces[name][:CAP, cols] for name in OWN], axis=0)
        total = weighed(mark_own, rows) + shared[:, cols]
        own_sum[:, cols] = total + jnp.where(core0, weighed(other, extra[:, cols]), 0.0)
        rows = [pieces[name][-2 * CAP : -CAP, cols] for name in NAMES]
        one_sum[:, cols] = weighed(mark_one, jnp.concatenate(rows, axis=0))


def ffn_kernel(rows_ref, gate_ref, up_ref, down_ref, out_ref):
    rows = rows_ref[...]
    gate_value = jnp.dot(rows, gate_ref[...], preferred_element_type=jnp.float32)
    up_value = jnp.dot(rows, up_ref[...], preferred_element_type=jnp.float32)
    activated = gate_value / (1.0 + jnp.exp(-gate_value)) * up_value
    activated = activated.astype(jnp.bfloat16)
    for cols in blocks(out_ref.shape[1]):
        out_ref[:, cols] = jnp.dot(
            activated, down_ref[:, cols], preferred_element_type=jnp.float32
        ).astype(out_ref.dtype)


def add_kernel(part_ref, other_ref, *outs):
    at = 0
    for ref in outs:
        rows = slice(at, at + ref.shape[0])
        ref[...] = (part_ref[rows, :] + other_ref[rows, :].astype(jnp.float32)).astype(jnp.bfloat16)
        at += ref.shape[0]


def away(value, shift):
    return moved(value, shift, -shift) if shift else value


def per_device(
    tokens,
    norm_gain,
    routes,
    route_weights,
    gate_experts,
    up_experts,
    down_experts,
    shared_gate,
    shared_up,
    shared_down,
    out_gain,
):
    tok_rows, width = tokens.shape
    n = lax.axis_size("ep")
    half_width = width // 2
    me = lax.axis_index("ep")
    core = lax.axis_index("tp")
    half = [bf16(tok_rows // 2, width + META)] * 2
    gain = norm_gain.astype(jnp.float32)[None, :]
    own = call(norm_kernel, half, [], [tokens, gain, routes.T, route_weights.T])

    last = n // 2 - 2 * STRIDE
    sign = 1 - 2 * core
    shifts = [sign * SHIFTS[name] for name in NAMES] + [jnp.where(core == 0, 0, -last)]
    ids = jnp.stack([(me + n + shift) % n for shift in shifts] + [core]).astype(jnp.int32)
    weights = gate_experts[0], up_experts[0], down_experts[0]

    one = [away(piece, STRIDE) for piece in own]
    two = [away(piece, STRIDE) for piece in one]
    marks = [(2, tok_rows, CAP * len(names)) for names in (OWN, NAMES, NAMES, ("extra",))]
    marks = [bf16(*shape) for shape in marks]
    outs = [bf16((SLOTS[name] - 1) * CAP, width) for name in NAMES]
    *early, mark_own, mark_one = call(select0_kernel, outs + marks[:2], [ids], [*own, *one])
    outs = [bf16(count * CAP, width) for count in SLOTS.values()]
    *pieces, extra, mark_two, other = call(
        select1_kernel, outs + marks[2:], [ids], [*own, *two, *early]
    )

    arrived = {"extra": jnp.where(core == 0, extra, moved(extra, None, -last))}
    for name, piece in reversed(list(zip(NAMES, pieces))):
        arrived[name] = away(piece, SHIFTS[name])
    mine = jnp.concatenate([arrived[name] for name in SLOTS], axis=0)
    theirs = swapped(mine)
    (my_part,) = call(ffn_kernel, [f32(*mine.shape)], [], [mine, *weights])
    (their_part,) = call(ffn_kernel, [bf16(*mine.shape)], [], [theirs, *weights])
    done = dict(zip(SLOTS, call(add_kernel, outs, [], [my_part, swapped(their_part)])))

    extra = jnp.where(core == 0, done["extra"], moved(done["extra"], None, last))
    back = {name: away(done[name], -SHIFTS[name]) for name in reversed(NAMES)}
    back = [back[name] for name in NAMES]
    sums = call(
        combine1_kernel, [bf16(tok_rows, half_width)] * 2, [ids], [mark_two, other, *back, extra]
    )
    came = [away(part, -STRIDE) for part in sums]
    normed = jnp.concatenate([piece[:, :width] for piece in own], axis=0)
    (shared,) = call(
        ffn_kernel, [f32(tok_rows, width)], [], [normed, shared_gate, shared_up, shared_down]
    )
    own_sum, one_sum = call(
        combine0_kernel,
        [f32(tok_rows, width)] * 2,
        [ids],
        [mark_own, mark_one, other, *back, extra, shared],
    )
    finals = []
    for c in range(2):
        cols = slice(c * half_width, (c + 1) * half_width)
        total = one_sum[:, cols] + came[c].astype(jnp.float32)
        total = away(total.astype(jnp.bfloat16), -STRIDE)
        finals.append(own_sum[:, cols] + total.astype(jnp.float32))
    final = jnp.concatenate(finals, axis=1)

    mixed = final + swapped(final.astype(jnp.bfloat16)).astype(jnp.float32)
    inverse = lax.rsqrt(jnp.mean(mixed * mixed, axis=1, keepdims=True) + EPS)
    kept = jnp.where(core == 0, mixed[:, :half_width], mixed[:, half_width:])
    return (kept * inverse * out_gain.astype(jnp.float32)[None, :]).astype(jnp.bfloat16)


def solution(mesh):
    in_specs = (
        P(("grp", "ep"), None),
        P(),
        P(("grp", "ep"), None),
        P(("grp", "ep"), None),
        P("ep", None, "tp"),
        P("ep", None, "tp"),
        P("ep", "tp", None),
        P(None, "tp"),
        P(None, "tp"),
        P("tp", None),
        P("tp"),
    )
    out_specs = P(("grp", "ep"), "tp")
    return jax.shard_map(
        per_device, mesh=mesh, in_specs=in_specs, out_specs=out_specs, check_vma=False
    )
```
